128 devices in a mesh: ep: 64 (over z, y, x), tp: 2 (over core).
Axes of the slice: x: 4, y: 4, z: 4, core: 2. Of those that a mesh axis runs over, the one named last changes fastest.
Arguments:
- tokens: bfloat16 [256, 4096], P('ep'), may hold values from -6 to 6
- memory: float32 [256, 8, 256, 512], P('ep', 'tp'), may hold values from -6 to 6
- normalizer: float32 [256, 8, 256], P('ep', 'tp'), may hold values from -6 to 6
- stabilizer: float32 [256, 8], P('ep', 'tp'), may hold values from -4 to 4
- norm_gain: float32 [4096], replicated, may hold values from 0.1 to 1.9
- w_query: bfloat16 [4096, 8, 256], P(None, 'tp', 'ep'), may hold values from -0.09375 to 0.09375
- w_key: bfloat16 [4096, 8, 256], P(None, 'tp', 'ep'), may hold values from -0.09375 to 0.09375
- w_value: bfloat16 [4096, 8, 512], P(None, 'tp', 'ep'), may hold values from -0.09375 to 0.09375
- w_outgate: bfloat16 [4096, 8, 512], P(None, 'tp', 'ep'), may hold values from -0.09375 to 0.09375
- w_input: bfloat16 [4096, 8], P(None, 'tp'), may hold values from -0.09375 to 0.09375
- w_forget: bfloat16 [4096, 8], P(None, 'tp'), may hold values from -0.09375 to 0.09375
- forget_bias: float32 [8], P('tp'), may hold values from 0 to 4
- w_out: bfloat16 [4096, 4096], P('tp', 'ep'), may hold values from -0.09375 to 0.09375
- ffn_gain: float32 [4096], replicated, may hold values from 0.1 to 1.9
- w_gate: bfloat16 [64, 4096, 512], P('ep', None, 'tp'), may hold values from -0.09375 to 0.09375
- w_up: bfloat16 [64, 4096, 512], P('ep', None, 'tp'), may hold values from -0.09375 to 0.09375
- w_down: bfloat16 [64, 512, 4096], P('ep', 'tp'), may hold values from -0.25 to 0.25
- expert_ids: int32 [256, 2], P('ep'), may hold values from 0 to 63, as said below
- route_weights: float32 [256, 2], P('ep'), may hold values from 0.1 to 1
Outputs:
- out: bfloat16 [256, 4096], P('ep')
- memory_next: float32 [256, 8, 256, 512], P('ep', 'tp')
- normalizer_next: float32 [256, 8, 256], P('ep', 'tp')
- stabilizer_next: float32 [256, 8], P('ep', 'tp')
The draws below stay inside these ranges and needn't reach their ends.
Inputs may be any that keep to these rules, and one draw needn't show every extreme that they name: `expert_ids`: the 2 experts of a token differ and lie in one group of 8 consecutive experts. Beyond that, any choice is allowed: for instance, all 4 tokens of one index of ep may name the same expert.
All inputs are finite; a program needn't handle non-finite values.
Results may differ from the reference program's by a relative error of at most 0.013.
Values may be sent and summed in bfloat16 or wider, within the bound.
A program may use at most 128 MiB of HBM per device.

```python
import jax
import jax.numpy as jnp
from jax import lax

D = 4096
HEADS = 8
DK = 256
DV = 512
DFF = 512
EXPERTS_PER_GROUP = 8
TOP = 2
SEQ_DEV = 4
SEQS = 256
EXPERTS = 64
GROUPS = 8
N_TP = 2


def draw_expert_ids(key, part):
    keys = jax.random.split(jax.random.fold_in(key, 7), 5)
    owner = jnp.arange(SEQS) // SEQ_DEV
    groups = jnp.minimum(jax.random.randint(keys[0], (SEQS,), 0, GROUPS), jax.random.randint(keys[1], (SEQS,), 0, GROUPS))
    first = jax.random.randint(keys[2], (SEQS,), 0, EXPERTS_PER_GROUP)
    offset = jax.random.randint(keys[3], (SEQS,), 1, EXPERTS_PER_GROUP)
    chosen = jax.random.randint(keys[4], (), 0, SEQS // SEQ_DEV)
    leader = chosen * SEQ_DEV
    groups = jnp.where(owner == chosen, groups[leader], groups)
    first = jnp.where(owner == chosen, first[leader], first)
    second = (first + offset) % EXPERTS_PER_GROUP
    return jnp.stack([groups * EXPERTS_PER_GROUP + first, groups * EXPERTS_PER_GROUP + second], axis=1).astype(jnp.int32)


def level_of(stream_key, shape, shards, least, high):
    def one(axis_at, blocks):
        heights = jax.random.uniform(jax.random.fold_in(jax.random.fold_in(stream_key, 6), axis_at), (blocks,), jnp.float32, least / len(shards), high / len(shards))
        return jnp.repeat(jnp.exp(heights), shape[axis_at] // blocks).reshape((-1,) + (1,) * (len(shape) - axis_at - 1))

    factor_of = one(*shards[0])
    for cut in shards[1:]:
        factor_of = factor_of * one(*cut)
    return factor_of


def gaussian(stream_key, shape, scale, most, cuts=(), held_as=jnp.bfloat16):
    entries = scale * jax.random.normal(stream_key, shape, jnp.float32)
    if cuts:
        entries = entries * level_of(stream_key, shape, cuts, -0.22, 0.18)
    return jnp.clip(entries, -most, most).astype(held_as)


def setup_inputs(seed: int = 0) -> dict:
    arg_keys = jax.random.split(jax.random.key(seed), 20)
    return {
        "tokens": gaussian(arg_keys[0], (SEQS, D), 1.0, 6.0, ((0, 64),)),
        "memory": gaussian(arg_keys[1], (SEQS, HEADS, DK, DV), 1.0, 6.0, ((0, 64), (1, 2)), jnp.float32),
        "normalizer": gaussian(arg_keys[2], (SEQS, HEADS, DK), 1.0, 6.0, ((0, 64), (1, 2)), jnp.float32),
        "stabilizer": gaussian(arg_keys[3], (SEQS, HEADS), 1.0, 4.0, ((0, 64), (1, 2)), jnp.float32),
        "norm_gain": jnp.clip(1.0 + 0.18 * jax.random.normal(arg_keys[4], (D,), jnp.float32), 0.1, 1.9),
        "w_query": gaussian(arg_keys[5], (D, HEADS, DK), D ** -0.5, 0.09375, ((1, 2), (2, 64))),
        "w_key": gaussian(arg_keys[6], (D, HEADS, DK), D ** -0.5, 0.09375, ((1, 2), (2, 64))),
        "w_value": gaussian(arg_keys[7], (D, HEADS, DV), D ** -0.5, 0.09375, ((1, 2), (2, 64))),
        "w_outgate": gaussian(arg_keys[8], (D, HEADS, DV), D ** -0.5, 0.09375, ((1, 2), (2, 64))),
        "w_input": gaussian(arg_keys[9], (D, HEADS), D ** -0.5, 0.09375, ((1, 2),)),
        "w_forget": gaussian(arg_keys[10], (D, HEADS), D ** -0.5, 0.09375, ((1, 2),)),
        "forget_bias": jnp.clip(4.0 * jax.random.uniform(arg_keys[11], (HEADS,), jnp.float32) ** level_of(arg_keys[11], (HEADS,), ((0, 2),), -0.2, 0.2), 0.0, 4.0),
        "w_out": gaussian(arg_keys[12], (HEADS * DV, D), (HEADS * DV) ** -0.5, 0.09375, ((0, 2), (1, 64))),
        "ffn_gain": jnp.clip(1.0 + 0.18 * jax.random.normal(arg_keys[13], (D,), jnp.float32), 0.1, 1.9),
        "w_gate": gaussian(arg_keys[14], (EXPERTS, D, DFF), D ** -0.5, 0.09375, ((0, 64), (2, 2))),
        "w_up": gaussian(arg_keys[15], (EXPERTS, D, DFF), D ** -0.5, 0.09375, ((0, 64), (2, 2))),
        "w_down": gaussian(arg_keys[16], (EXPERTS, DFF, D), DFF ** -0.5, 0.25, ((0, 64), (1, 2))),
        "expert_ids": draw_expert_ids(jax.random.fold_in(arg_keys[19], 71), 0),
        "route_weights": jnp.clip(0.1 + 0.9 * jax.random.uniform(arg_keys[18], (SEQS, TOP), jnp.float32) ** level_of(arg_keys[18], (SEQS, TOP), ((0, 64),), -0.2, 0.2), 0.1, 1.0),
    }


def rms_scale(values, gain):
    return values * lax.rsqrt(lax.optimization_barrier(jnp.mean(values * values, axis=-1, keepdims=True)) + 1e-06) * gain

def product(left, right):
    return jnp.dot(left, right, preferred_element_type=jnp.float32)

def rounded_term(values):
    return lax.optimization_barrier(values.astype(jnp.bfloat16)).astype(jnp.float32)

def cell_step(inputs):
    memory, normalizer, stabilizer, scaled, key, value, in_pre, log_forget = inputs
    stab_next = jnp.maximum(log_forget + stabilizer, in_pre)
    decay = jnp.exp(log_forget + stabilizer - stab_next)
    inweight = jnp.exp(in_pre - stab_next)
    memory_next = decay[:, None, None] * memory + inweight[:, None, None] * (key[:, :, None] * value[:, None, :])
    normalizer_next = decay[:, None] * normalizer + inweight[:, None] * key
    numerator = jnp.einsum('hd,hde->he', scaled, memory_next, precision=lax.Precision.HIGHEST)
    denominator = lax.optimization_barrier(jnp.sum(scaled * normalizer_next, axis=-1))
    hidden = numerator / jnp.maximum(jnp.abs(denominator), jnp.exp(-stab_next))[:, None]
    return (memory_next, normalizer_next, stab_next, hidden)

def reference(tokens, memory, normalizer, stabilizer, norm_gain, w_query, w_key, w_value, w_outgate, w_input, w_forget, forget_bias, w_out, ffn_gain, w_gate, w_up, w_down, expert_ids, route_weights):
    seqs = tokens.shape[0]
    normed = rms_scale(tokens.astype(jnp.float32), norm_gain).astype(jnp.bfloat16)
    query = product(normed, w_query.reshape(D, HEADS * DK)).astype(jnp.bfloat16)
    key = product(normed, w_key.reshape(D, HEADS * DK)).astype(jnp.bfloat16)
    value = product(normed, w_value.reshape(D, HEADS * DV)).astype(jnp.bfloat16)
    outgate = product(normed, w_outgate.reshape(D, HEADS * DV)).astype(jnp.bfloat16)
    in_pre = product(normed, w_input)
    log_forget = jax.nn.log_sigmoid(product(normed, w_forget) + forget_bias)
    scaled = query.astype(jnp.float32).reshape(seqs, HEADS, DK) * DK ** (-0.5)
    key_heads = key.astype(jnp.float32).reshape(seqs, HEADS, DK)
    value_heads = value.astype(jnp.float32).reshape(seqs, HEADS, DV)
    memory_next, normalizer_next, stab_next, hidden = lax.map(cell_step, (memory, normalizer, stabilizer, scaled, key_heads, value_heads, in_pre, log_forget))
    hidden = (hidden.reshape(seqs, HEADS * DV) * jax.nn.sigmoid(outgate.astype(jnp.float32))).astype(jnp.bfloat16)
    span = HEADS * DV // N_TP
    mixed = jnp.zeros((seqs, D), jnp.float32)
    for member in range(N_TP):
        mixed = mixed + rounded_term(product(hidden[:, member * span:(member + 1) * span], w_out[member * span:(member + 1) * span]))
    mixed = mixed.astype(jnp.bfloat16)
    resid = tokens.astype(jnp.float32) + mixed.astype(jnp.float32)
    ffn_in = rms_scale(resid, ffn_gain).astype(jnp.bfloat16)
    hidden_span = DFF // N_TP

    def expert_row(inputs):
        row, expert, weight = inputs
        gate_part = product(row, w_gate[expert])
        up_part = product(row, w_up[expert])
        act = (jax.nn.silu(gate_part) * up_part).astype(jnp.bfloat16)
        down = w_down[expert]
        total = jnp.zeros((D,), jnp.float32)
        for member in range(N_TP):
            total = total + weight * rounded_term(product(act[member * hidden_span:(member + 1) * hidden_span], down[member * hidden_span:(member + 1) * hidden_span]))
        return total
    rows = jnp.repeat(ffn_in, TOP, axis=0)
    weighted = lax.map(expert_row, (rows, expert_ids.reshape(-1).astype(jnp.int32), route_weights.reshape(-1)))
    ffn_out = lax.optimization_barrier(jnp.sum(weighted.reshape(seqs, TOP, D), axis=1))
    out = (resid + ffn_out).astype(jnp.bfloat16)
    return (out, memory_next, normalizer_next, stab_next)
```

```python
import functools

import jax
import jax.numpy as jnp
from jax import lax
from jax.experimental import pallas as pl
from jax.experimental.pallas import tpu as pltpu
from jax.sharding import PartitionSpec as P

MESH = pl.DeviceIdType.MESH
F32 = jnp.float32
BF16 = jnp.bfloat16
STRIDE = {"x": 1, "y": 4, "z": 16}
SEND_ORDER = (1, 3, 2)


def place():
    ep = lax.axis_index("ep")
    at = {"x": lax.rem(ep, 4), "y": lax.rem(ep // 4, 4), "z": ep // 16}
    return ep, lax.axis_index("tp"), at


def shifted(at, axis, offset):
    return lax.rem(at[axis] + 4 + offset, 4)


def peer(ep, at, axis, offset):
    return ep + (shifted(at, axis, offset) - at[axis]) * STRIDE[axis]


def remote(src, dst, send, recv, ep, tp):
    return pltpu.make_async_remote_copy(
        src_ref=src, dst_ref=dst, send_sem=send, recv_sem=recv, device_id=(ep, tp), device_id_type=MESH
    )


def greet(ep, tp, at):
    barrier = pltpu.get_barrier_semaphore()
    for axis in "xyz":
        for o in (1, 2, 3):
            pl.semaphore_signal(barrier, inc=1, device_id=(peer(ep, at, axis, o), tp), device_id_type=MESH)
    pl.semaphore_signal(barrier, inc=1, device_id=(ep, 1 - tp), device_id_type=MESH)


def met():
    pl.semaphore_wait(pltpu.get_barrier_semaphore(), 10)


AXES = (("y", "z"), ("z", "y"))


def line_of(at, part, m, n):
    first, second = AXES[part]
    c = {first: shifted(at, first, -m), second: shifted(at, second, -n)}
    return c["z"] * 4 + c["y"]


def spread_x(ep, tp, at, own, slot, s1, r1):
    for o in SEND_ORDER:
        remote(own, slot(at["x"]), s1.at[o], r1.at[o], peer(ep, at, "x", o), tp).start()


def spread_x_wait(ep, tp, at, own, slot, s1, r1):
    for o in SEND_ORDER:
        remote(own, slot(shifted(at, "x", -o)), s1.at[o], r1.at[o], ep, tp).wait_recv()


def spread_x_end(ep, tp, at, own, slot, s1, r1):
    for o in SEND_ORDER:
        remote(own, slot(at["x"]), s1.at[o], r1.at[o], ep, tp).wait_send()


def lines_relay(ep, tp, at, ref, part, m, n, pair):
    if pair is not None:
        here = ref(line_of(at, part, m, n), part)
        remote(here, here, pair[0].at[part, m, n], pair[1].at[part, m, n], ep, 1 - tp).start()


def lines_onward(ep, tp, at, ref, part, m, s3, r3):
    here = ref(line_of(at, part, m, 0), part)
    for o in SEND_ORDER:
        remote(here, here, s3.at[part, m, o], r3.at[part, m, o], peer(ep, at, AXES[part][1], o), tp).start()


def spread_lines_early(ep, tp, at, ref, s2, r2, s3, r3, pair=None):
    for part in range(2):
        here = ref(line_of(at, part, 0, 0), part)
        for o in SEND_ORDER:
            remote(here, here, s2.at[part, o], r2.at[part, o], peer(ep, at, AXES[part][0], o), tp).start()
    for part in range(2):
        lines_onward(ep, tp, at, ref, part, 0, s3, r3)
        lines_relay(ep, tp, at, ref, part, 0, 0, pair)


def spread_lines_late(ep, tp, at, ref, s2, r2, s3, r3, pair=None, seen=None):
    for m in SEND_ORDER:
        for part in range(2):
            here = ref(line_of(at, part, m, 0), part)
            remote(here, here, s2.at[part, m], r2.at[part, m], ep, tp).wait_recv()
            lines_onward(ep, tp, at, ref, part, m, s3, r3)
            lines_relay(ep, tp, at, ref, part, m, 0, pair)
            if seen is not None:
                seen(part, line_of(at, part, m, 0))
    for m in (0, 1, 3, 2):
        for o in SEND_ORDER:
            for part in range(2):
                here = ref(line_of(at, part, m, o), part)
                remote(here, here, s3.at[part, m, o], r3.at[part, m, o], ep, tp).wait_recv()
                lines_relay(ep, tp, at, ref, part, m, o, pair)
                if seen is not None:
                    seen(part, line_of(at, part, m, o))


def spread_lines_pair_wait(ep, tp, at, other, pair):
    for part in range(2):
        for m in range(4):
            for n in range(4):
                here = other(line_of(at, part, m, n), part)
                remote(here, here, pair[0].at[part, m, n], pair[1].at[part, m, n], ep, 1 - tp).wait_recv()


def spread_lines_end(ep, tp, at, ref, s2, r2, s3, r3, pair=None):
    here0 = [ref(line_of(at, part, 0, 0), part) for part in range(2)]
    for part in range(2):
        here = here0[part]
        for o in SEND_ORDER:
            remote(here, here, s2.at[part, o], r2.at[part, o], ep, tp).wait_send()
        for m in range(4):
            for o in SEND_ORDER:
                remote(here, here, s3.at[part, m, o], r3.at[part, m, o], ep, tp).wait_send()
            if pair is not None:
                for n in range(4):
                    remote(here, here, pair[0].at[part, m, n], pair[1].at[part, m, n], ep, 1 - tp).wait_send()


def part_cols(part, width):
    return pl.ds(part * width, width)


def kernel_a(
    tok_ref, gain_ref, ids_ref, rw_ref, wq_hbm, wk_hbm, wv_hbm, wo_hbm,
    recv_ref, all_ref,
    xblk, wq, wk, wv, wo, wt, acc, squares, slab,
    wsem, s1, r1, s2, r2, s3, r3, ps, pr, sa, ra,
):
    ep, tp, at = place()
    greet(ep, tp, at)
    loads = [
        pltpu.make_async_copy(src, dst, wsem.at[n])
        for n, (src, dst) in enumerate(((wq_hbm, wq), (wk_hbm, wk), (wv_hbm, wv), (wo_hbm, wo)))
    ]
    for load in loads:
        load.start()
    half = 2048
    own = tok_ref.at[:, pl.ds(pl.multiple_of(tp * half, 128), half)]
    met()
    slot = lambda x: xblk.at[x]
    spread_x(ep, tp, at, own, slot, s1, r1)
    xblk[at["x"]] = tok_ref[:, pl.ds(pl.multiple_of(tp * half, 128), half)]
    spread_x_wait(ep, tp, at, own, slot, s1, r1)
    mine = at["z"] * 4 + at["y"]
    for n in range(0, half, 512):
        cols = pl.ds(n, 512)
        all_ref[tp, mine, :, cols] = jnp.concatenate([xblk[x, :, cols].astype(F32) for x in range(4)], axis=0).astype(BF16)
    ref = lambda line, part: all_ref.at[tp, line, :, part_cols(part, half // 2)]
    other = lambda line, part: all_ref.at[1 - tp, line, :, part_cols(part, half // 2)]
    lines = (ep, tp, at, ref, s2, r2, s3, r3, (ps, pr))
    spread_lines_early(*lines)
    for load in loads:
        load.wait()
    wt[96:128, :] = jnp.zeros((32, 4096), BF16)
    for n in range(0, 4096, 1024):
        cols = pl.ds(n, 1024)
        for row, tall, w in ((0, 16, wq), (16, 16, wk), (32, 32, wv), (64, 32, wo)):
            wt[row : row + tall, cols] = jnp.concatenate([w[h, :, cols].astype(F32) for h in range(4)], axis=0).astype(BF16)

    squares[...] = jnp.zeros((16, 16, 128), F32)

    def measured(side, part, line):
        total = squares[line]
        for n in range(0, half // 2, 128):
            v = all_ref[side, line, :, pl.ds(part * (half // 2) + n, 128)].astype(F32)
            total += v * v
        squares[line] = total

    for part in range(2):
        measured(tp, part, mine)
    spread_lines_late(*lines, seen=lambda part, line: measured(tp, part, line))
    for part in range(2):
        for m in range(4):
            for n in range(4):
                line = line_of(at, part, m, n)
                here = other(line, part)
                remote(here, here, ps.at[part, m, n], pr.at[part, m, n], ep, 1 - tp).wait_recv()
                measured(1 - tp, part, line)
    mean = jnp.sum(squares[...].reshape(256, 128), axis=-1, keepdims=True) * (1.0 / 4096)
    scale = lax.rsqrt(mean + 1e-06)
    for n in range(0, 4096, 1024):
        cols = pl.ds(n, 1024)
        x = all_ref[n // half, :, :, pl.ds(n % half, 1024)].reshape(256, 1024).astype(F32)
        normed = (x * scale * gain_ref[:, cols]).astype(BF16)
        term = lax.dot_general(normed, wt[:, cols], (((1,), (1,)), ((), ())), preferred_element_type=F32)
        if n == 0:
            acc[...] = term
        else:
            acc[...] += term
    lane = lax.broadcasted_iota(jnp.int32, (4, 128), 1)
    diagonal = lax.broadcasted_iota(jnp.int32, (4, 4), 0) == lax.broadcasted_iota(jnp.int32, (4, 4), 1)
    upright = lambda row: jnp.sum(jnp.where(diagonal, row, 0.0), axis=1, keepdims=True)
    ids = ids_ref[...].astype(F32)
    id0, id1 = upright(ids[0:1]), upright(ids[1:2])
    rw0, rw1 = upright(rw_ref[0:1, :]), upright(rw_ref[1:2, :])
    for pairs in range(32):
        eight = acc[8 * pairs : 8 * pairs + 8, :]
        for k in range(2):
            e = 2 * pairs + k
            weight = jnp.where(id0 == float(e), rw0, 0.0) + jnp.where(id1 == float(e), rw1, 0.0)
            slab[e] = jnp.where(lane < 96, eight[4 * k : 4 * k + 4], jnp.where(lane == 96, weight, 0.0))

    @pl.loop(1, 64)
    def _(o):
        to = ep ^ o
        remote(slab.at[to], recv_ref.at[ep], sa.at[o], ra.at[o], to, tp).start()

    recv_ref[ep] = slab[ep]
    spread_x_end(ep, tp, at, own, slot, s1, r1)
    spread_lines_end(*lines)

    @pl.loop(1, 64)
    def _(o):
        remote(slab.at[ep ^ o], recv_ref.at[ep ^ o], sa.at[o], ra.at[o], ep ^ o, tp).wait()


def log_sigmoid(v):
    return -(jnp.maximum(-v, 0.0) + jnp.log1p(jnp.exp(-jnp.abs(v))))


def one_hot(rows, cols, test):
    r = lax.broadcasted_iota(jnp.int32, (rows, cols), 0)
    c = lax.broadcasted_iota(jnp.int32, (rows, cols), 1)
    return test(r, c)


def kernel_b(
    recv_ref, tok_ref, gain_ref, win_ref, wfg_ref, fbias_ref, stab_ref, nrm_ref, mem_hbm,
    memn_hbm, nrmn_ref, stabn_ref, hid_ref,
    buf, kq, hids, isem, osem,
):
    ins = [pltpu.make_async_copy(mem_hbm.at[n // 4, n % 4], buf.at[n], isem.at[n]) for n in range(16)]
    outs = [pltpu.make_async_copy(buf.at[n], memn_hbm.at[n // 4, n % 4], osem.at[n]) for n in range(16)]
    for copy in ins:
        copy.start()
    x = tok_ref[...].astype(F32)
    scale = lax.rsqrt(jnp.mean(x * x, axis=-1, keepdims=True) + 1e-06)
    normed = (x * scale * gain_ref[...]).astype(BF16).astype(F32)
    lane = lax.broadcasted_iota(jnp.int32, (4, 4), 1)
    in_pre = jnp.zeros((4, 4), F32)
    forget = jnp.zeros((4, 4), F32)
    for h in range(4):
        i_h = jnp.sum(normed * win_ref[h : h + 1, :].astype(F32), axis=-1, keepdims=True)
        f_h = jnp.sum(normed * wfg_ref[h : h + 1, :].astype(F32), axis=-1, keepdims=True)
        in_pre = jnp.where(lane == h, i_h, in_pre)
        forget = jnp.where(lane == h, f_h, forget)
    log_forget = log_sigmoid(forget + fbias_ref[...])
    held = log_forget + stab_ref[...]
    stab_next = jnp.maximum(held, in_pre)
    decay = jnp.exp(held - stab_next)
    inweight = jnp.exp(in_pre - stab_next)
    floor = jnp.exp(-stab_next)
    stabn_ref[...] = stab_next

    e4 = one_hot(256, 64, lambda r, c: r // 4 == c).astype(BF16)
    e8 = one_hot(512, 64, lambda r, c: r // 8 == c).astype(BF16)
    keep4 = one_hot(256, 128, lambda r, c: (r % 4 == c % 4) & (c < 32))
    keep8 = one_hot(512, 128, lambda r, c: (r % 8 == c % 8) & (c >= 32) & (c < 96))
    vo_cols = jnp.zeros((512, 128), F32)
    qk_cols = jnp.zeros((256, 128), F32)
    wide = []
    for h in range(4):
        wide.append(one_hot(128, 256, lambda r, c: (r // 4 == jnp.where(c < 128, 4 + h, h)) & (r < 32)).astype(BF16))
    for t in range(4):
        rows = recv_ref[pl.ds(t, 64, stride=4), :].astype(BF16)
        y4 = jnp.where(keep4, jnp.dot(e4, rows, preferred_element_type=F32), 0.0).astype(BF16)
        y8 = jnp.where(keep8, jnp.dot(e8, rows, preferred_element_type=F32), 0.0).astype(BF16)
        for h in range(4):
            kq[t * 4 + h] = jnp.dot(y4, wide[h], preferred_element_type=F32)
        f4 = one_hot(128, 128, lambda r, c: (c == t * 8 + r // 4) & (r < 32)).astype(BF16)
        f8 = one_hot(128, 128, lambda r, c: (c == t * 8 + (r - 32) // 8) & (r >= 32) & (r < 96)).astype(BF16)
        qk_cols += jnp.dot(y4, f4, preferred_element_type=F32)
        vo_cols += jnp.dot(y8, f8, preferred_element_type=F32)
    qk_rows = qk_cols.T
    vo_rows = vo_cols.T
    for n in range(16):
        t, h = n // 4, n % 4
        d = decay[t : t + 1, h : h + 1]
        w = inweight[t : t + 1, h : h + 1]
        q_row = qk_rows[t * 8 + h : t * 8 + h + 1, :] * 0.0625
        k_row = qk_rows[t * 8 + 4 + h : t * 8 + 5 + h, :]
        v_row = vo_rows[t * 8 + h : t * 8 + h + 1, :]
        o_row = vo_rows[t * 8 + 4 + h : t * 8 + 5 + h, :]
        norm_next = d * nrm_ref[t, h : h + 1, :] + w * k_row
        nrmn_ref[t, h : h + 1, :] = norm_next
        den = jnp.sum(q_row * norm_next, axis=-1, keepdims=True)
        ins[n].wait()
        d_all = jnp.broadcast_to(d, (8, 128))
        vs = [jnp.broadcast_to(w * v_row[:, 128 * c : 128 * c + 128], (8, 128)) for c in range(4)]

        def step(r, total, n=n, d_all=d_all, vs=vs):
            total = list(total)
            for g in range(4):
                rows = pl.ds(pl.multiple_of(r * 32 + 8 * g, 8), 8)
                k_all = kq[n, rows, 0:128]
                q_all = kq[n, rows, 128:256]
                for c in range(4):
                    cols = slice(128 * c, 128 * c + 128)
                    new = d_all * buf[n, rows, cols] + k_all * vs[c]
                    buf[n, rows, cols] = new
                    total[c] = total[c] + q_all * new
            return tuple(total)

        total = lax.fori_loop(0, 8, step, tuple(jnp.zeros((8, 128), F32) for _ in range(4)))
        outs[n].start()
        numer = jnp.sum(jnp.concatenate(total, axis=1), axis=0, keepdims=True) * 0.0625
        hidden = numer / jnp.maximum(jnp.abs(den), floor[t : t + 1, h : h + 1]) * jax.nn.sigmoid(o_row)
        hids[t : t + 1, h * 512 : (h + 1) * 512] = hidden
    hid_ref[...] = hids[...].astype(BF16)
    for copy in outs:
        copy.wait()


def kernel_c(
    hid_ref, recv_ref, gain_ref, tok_hbm, wo_hbm, wg_hbm, wu_hbm, wd_hbm,
    out_ref,
    xblk, hall, wo, toks, wg, wu, wd, pk, pr_in, mall, resid, resid_own, gate, up, act, away, back, terms,
    r1buf, s1buf, r2buf, xsend, xrecv, ends,
    wsem, s1, r1, s2, r2, s3, r3, ms1, mr1, ms2, mr2, ms3, mr3, mps, mpr, dps, dpr, hs, hr,
    q1s, q1r, q2s, q2r, q3s, q3r, fs, fr,
):
    ep, tp, at = place()
    greet(ep, tp, at)
    loads = [
        pltpu.make_async_copy(src, dst, wsem.at[n])
        for n, (src, dst) in enumerate(((wo_hbm, wo), (tok_hbm, toks), (wg_hbm, wg), (wu_hbm, wu), (wd_hbm, wd)))
    ]
    for load in loads:
        load.start()
    half = 2048
    mine = at["z"] * 4 + at["y"]
    met()
    slot = lambda x: xblk.at[x]
    spread_x(ep, tp, at, hid_ref, slot, s1, r1)
    xblk[at["x"]] = hid_ref[...]
    spread_x_wait(ep, tp, at, hid_ref, slot, s1, r1)
    for n in range(0, half, 512):
        cols = pl.ds(n, 512)
        hall[mine, :, cols] = jnp.concatenate([xblk[x, :, cols].astype(F32) for x in range(4)], axis=0).astype(BF16)
    href = lambda line, part: hall.at[line, :, part_cols(part, half // 2)]
    hidden_lines = (ep, tp, at, href, s2, r2, s3, r3)
    spread_lines_early(*hidden_lines)
    for load in loads:
        load.wait()
    spread_lines_late(*hidden_lines)

    term = jnp.zeros((256, 64), F32)
    for n in range(0, half, 512):
        term += lax.dot_general(
            hall[:, :, pl.ds(n, 512)].reshape(256, 512), wo[:, pl.ds(n, 512)],
            (((1,), (1,)), ((), ())), preferred_element_type=F32,
        )
    for p in range(2):
        pk[p] = jnp.concatenate([term[128 * p : 128 * p + 64], term[128 * p + 64 : 128 * p + 128]], axis=1).astype(BF16)
    swap = remote(pk.at[1 - tp], pr_in, hs, hr, ep, 1 - tp)
    swap.start()
    spread_x_end(ep, tp, at, hid_ref, slot, s1, r1)
    spread_lines_end(*hidden_lines)
    swap.wait()
    mall[tp, mine, at["x"]] = (pk[tp].astype(F32) + pr_in[...].astype(F32)).astype(BF16)
    own = mall.at[tp, mine, at["x"]]
    mslot = lambda x: mall.at[tp, mine, x]
    spread_x(ep, tp, at, own, mslot, ms1, mr1)
    spread_x_wait(ep, tp, at, own, mslot, ms1, mr1)
    mref = lambda line, part: mall.at[tp, line, :, pl.ds(32 * part, 32), :]
    mother = lambda line, part: mall.at[1 - tp, line, :, pl.ds(32 * part, 32), :]
    mixed_lines = (ep, tp, at, mref, ms2, mr2, ms3, mr3, (mps, mpr))
    spread_lines_early(*mixed_lines)
    spread_lines_late(*mixed_lines)
    spread_lines_pair_wait(ep, tp, at, mother, (mps, mpr))

    low = lax.broadcasted_iota(jnp.int32, (64, 128), 1) < 64
    scales = []
    for p in range(2):

        def pair_of_chips(jj, sums, p=p):
            a = mall[p, jj // 2, 2 * lax.rem(jj, 2)].astype(F32)
            b = mall[p, jj // 2, 2 * lax.rem(jj, 2) + 1].astype(F32)
            mixes = (jnp.where(low, a, pltpu.roll(b, 64, 1)), jnp.where(low, pltpu.roll(a, 64, 1), b))
            cols = pl.ds(pl.multiple_of(128 * jj, 128), 128)
            tcols = pl.ds(pl.multiple_of(128 * lax.rem(jj, 16), 128), 128)
            new = []
            for k in range(2):
                row = 128 * p + 64 * k
                r = toks[jj // 16, row // 16 : row // 16 + 4, :, tcols].reshape(64, 128).astype(F32) + mixes[k]
                resid[row : row + 64, cols] = r
                new.append(sums[k] + r * r)
            return tuple(new)

        sums = lax.fori_loop(0, 32, pair_of_chips, (jnp.zeros((64, 128), F32), jnp.zeros((64, 128), F32)))
        for k in range(2):
            scales.append(lax.rsqrt(jnp.sum(sums[k], axis=-1, keepdims=True) * (1.0 / 4096) + 1e-06))
    scale = jnp.concatenate(scales, axis=0)
    my_cols = pl.ds(pl.multiple_of(tp * half, 128), half)
    eight = resid[pl.ds(pl.multiple_of(8 * (ep // 2), 8), 8), my_cols]
    resid_own[...] = jnp.where(lax.rem(ep, 2) == 0, eight[0:4], eight[4:8])

    for n in range(0, 4096, 1024):
        cols = pl.ds(n, 1024)
        x = (resid[:, cols] * scale * gain_ref[:, cols]).astype(BF16)
        g = jnp.dot(x, wg[cols, :], preferred_element_type=F32)
        u = jnp.dot(x, wu[cols, :], preferred_element_type=F32)
        if n == 0:
            gate[...] = g
            up[...] = u
        else:
            gate[...] += g
            up[...] += u
    g = gate[...]
    act[...] = (g * jax.nn.sigmoid(g) * up[...]).astype(BF16)
    weight = recv_ref[:, 96:97]

    def weighted(cols):
        t = jnp.dot(act[...], wd[:, cols], preferred_element_type=F32)
        return t.astype(BF16).astype(F32) * weight

    swaps = []
    for n in range(4):
        here = pl.ds(512 * n, 512)
        cols = pl.ds(pl.multiple_of((1 - tp) * half + 512 * n, 128), 512)
        away[:, :, here] = weighted(cols).astype(BF16).reshape(16, 16, 512)
        copy = remote(away.at[:, :, here], back.at[:, :, here], dps.at[n], dpr.at[n], ep, 1 - tp)
        copy.start()
        swaps.append(copy)
    spread_x_end(ep, tp, at, own, mslot, ms1, mr1)
    spread_lines_end(*mixed_lines)
    for n in range(4):
        here = pl.ds(512 * n, 512)
        cols = pl.ds(pl.multiple_of(tp * half + 512 * n, 128), 512)
        mine_term = weighted(cols)
        swaps[n].wait_recv()
        terms[:, :, :, here] = (mine_term + back[:, :, here].reshape(256, 512).astype(F32)).astype(BF16).reshape(4, 4, 16, 512)
        if n % 2 == 1:
            part = n // 2
            axis = ("z", "y")[part]
            for o in SEND_ORDER:
                c = shifted(at, axis, o)
                src = terms.at[c, :, :, part_cols(0, 1024)] if part == 0 else terms.at[:, c, :, part_cols(1, 1024)]
                remote(src, r1buf.at[part, o], q1s.at[part, o], q1r.at[part, o], peer(ep, at, axis, o), tp).start()

    own1 = lambda part, cols: terms[at["z"], :, :, cols] if part == 0 else terms[:, at["y"], :, cols]
    for part in range(2):
        for o in SEND_ORDER:
            remote(s1buf.at[part], r1buf.at[part, o], q1s.at[part, o], q1r.at[part, o], ep, tp).wait_recv()
        for n in range(0, 1024, 256):
            total = own1(part, pl.ds(part * 1024 + n, 256)).astype(F32)
            for o in (1, 2, 3):
                total += r1buf[part, o, :, :, pl.ds(n, 256)].astype(F32)
            s1buf[part, :, :, pl.ds(n, 256)] = total.astype(BF16)
        axis = ("y", "z")[part]
        for o in SEND_ORDER:
            c = shifted(at, axis, o)
            remote(s1buf.at[part, c], r2buf.at[part, o], q2s.at[part, o], q2r.at[part, o], peer(ep, at, axis, o), tp).start()
    for part in range(2):
        for o in SEND_ORDER:
            remote(s1buf.at[part, 0], r2buf.at[part, o], q2s.at[part, o], q2r.at[part, o], ep, tp).wait_recv()
        for n in range(0, 1024, 512):
            total = s1buf[part, at[("y", "z")[part]], :, pl.ds(n, 512)].astype(F32)
            for o in (1, 2, 3):
                total += r2buf[part, o, :, pl.ds(n, 512)].astype(F32)
            for x in range(4):
                xsend[x, :, pl.ds(part * 1024 + n, 512)] = total[4 * x : 4 * x + 4].astype(BF16)
    for o in SEND_ORDER:
        remote(xsend.at[shifted(at, "x", o)], xrecv.at[o], q3s.at[o], q3r.at[o], peer(ep, at, "x", o), tp).start()
    total = xsend[at["x"]].astype(F32)
    for o in SEND_ORDER:
        remote(xsend.at[0], xrecv.at[o], q3s.at[o], q3r.at[o], ep, tp).wait_recv()
        total += xrecv[o].astype(F32)
    ends[tp] = (resid_own[...] + total).astype(BF16)
    last = remote(ends.at[tp], ends.at[tp], fs, fr, ep, 1 - tp)
    last.start()
    for n in range(4):
        swaps[n].wait_send()
    for part in range(2):
        for o in SEND_ORDER:
            remote(s1buf.at[part], r1buf.at[part, o], q1s.at[part, o], q1r.at[part, o], ep, tp).wait_send()
            remote(s1buf.at[part, 0], r2buf.at[part, o], q2s.at[part, o], q2r.at[part, o], ep, tp).wait_send()
    for o in SEND_ORDER:
        remote(xsend.at[0], xrecv.at[o], q3s.at[o], q3r.at[o], ep, tp).wait_send()
    last.wait_send()
    remote(ends.at[1 - tp], ends.at[1 - tp], fs, fr, ep, 1 - tp).wait_recv()
    for k in range(2):
        out_ref[:, k * half : (k + 1) * half] = ends[k]


V = pl.BlockSpec(memory_space=pltpu.VMEM)
ANY = pl.BlockSpec(memory_space=pl.ANY)
DMA = pltpu.SemaphoreType.DMA


def shape(dims, dtype):
    return jax.ShapeDtypeStruct(dims, dtype)


def call_a(tokens, gain, ids, rw, wq, wk, wv, wo):
    return pl.pallas_call(
        kernel_a,
        name="gather_project",
        out_shape=(shape((64, 4, 128), F32), shape((2, 16, 16, 2048), BF16)),
        in_specs=[V, V, V, V, ANY, ANY, ANY, ANY],
        out_specs=(V, V),
        scratch_shapes=[
            pltpu.VMEM((4, 4, 2048), BF16),
            pltpu.VMEM((4, 4, 4096), BF16),
            pltpu.VMEM((4, 4, 4096), BF16),
            pltpu.VMEM((4, 8, 4096), BF16),
            pltpu.VMEM((4, 8, 4096), BF16),
            pltpu.VMEM((128, 4096), BF16),
            pltpu.VMEM((256, 128), F32),
            pltpu.VMEM((16, 16, 128), F32),
            pltpu.VMEM((64, 4, 128), F32),
            DMA((4,)),
            DMA((4,)), DMA((4,)),
            DMA((2, 4)), DMA((2, 4)),
            DMA((2, 4, 4)), DMA((2, 4, 4)),
            DMA((2, 4, 4)), DMA((2, 4, 4)),
            DMA((64,)), DMA((64,)),
        ],
        compiler_params=pltpu.CompilerParams(collective_id=0, has_side_effects=True),
        cost_estimate=pl.CostEstimate(flops=10**9, bytes_accessed=10**7, transcendentals=0),
    )(tokens, gain, ids, rw, wq, wk, wv, wo)


def call_b(recv, tokens, gain, win, wfg, fbias, stab, nrm, mem):
    return pl.pallas_call(
        kernel_b,
        name="cell",
        out_shape=(
            shape(mem.shape, F32), shape(nrm.shape, F32), shape(stab.shape, F32), shape((4, 2048), BF16),
        ),
        in_specs=[V, V, V, V, V, V, V, V, ANY],
        out_specs=(ANY, V, V, V),
        scratch_shapes=[
            pltpu.VMEM((16, 256, 512), F32),
            pltpu.VMEM((16, 256, 256), F32),
            pltpu.VMEM((4, 2048), F32),
            DMA((16,)), DMA((16,)),
        ],
        compiler_params=pltpu.CompilerParams(),
        cost_estimate=pl.CostEstimate(flops=10**8, bytes_accessed=2 * 10**7, transcendentals=0),
    )(recv, tokens, gain, win, wfg, fbias, stab, nrm, mem)


def call_c(hidden, recv, gain, gathered, wo, wg, wu, wd):
    lines = lambda: [DMA((4,)), DMA((4,)), DMA((2, 4)), DMA((2, 4)), DMA((2, 4, 4)), DMA((2, 4, 4))]
    return pl.pallas_call(
        kernel_c,
        name="experts",
        out_shape=shape((4, 4096), BF16),
        in_specs=[V, V, V, ANY, ANY, ANY, ANY, ANY],
        out_specs=V,
        scratch_shapes=[
            pltpu.VMEM((4, 4, 2048), BF16),
            pltpu.VMEM((16, 16, 2048), BF16),
            pltpu.VMEM((64, 2048), BF16),
            pltpu.VMEM((2, 16, 16, 2048), BF16),
            pltpu.VMEM((4096, 256), BF16),
            pltpu.VMEM((4096, 256), BF16),
            pltpu.VMEM((256, 4096), BF16),
            pltpu.VMEM((2, 64, 128), BF16),
            pltpu.VMEM((64, 128), BF16),
            pltpu.VMEM((2, 16, 4, 64, 128), BF16),
            pltpu.VMEM((256, 4096), F32),
            pltpu.VMEM((4, 2048), F32),
            pltpu.VMEM((256, 256), F32),
            pltpu.VMEM((256, 256), F32),
            pltpu.VMEM((256, 256), BF16),
            pltpu.VMEM((16, 16, 2048), BF16),
            pltpu.VMEM((16, 16, 2048), BF16),
            pltpu.VMEM((4, 4, 16, 2048), BF16),
            pltpu.VMEM((2, 4, 4, 16, 1024), BF16),
            pltpu.VMEM((2, 4, 16, 1024), BF16),
            pltpu.VMEM((2, 4, 16, 1024), BF16),
            pltpu.VMEM((4, 4, 2048), BF16),
            pltpu.VMEM((4, 4, 2048), BF16),
            pltpu.VMEM((2, 4, 2048), BF16),
            DMA((5,)),
            *lines(),
            *lines(), DMA((2, 4, 4)), DMA((2, 4, 4)),
            DMA((4,)), DMA((4,)), DMA(()), DMA(()),
            DMA((2, 4)), DMA((2, 4)), DMA((2, 4)), DMA((2, 4)), DMA((4,)), DMA((4,)), DMA(()), DMA(()),
        ],
        compiler_params=pltpu.CompilerParams(collective_id=1, has_side_effects=True),
        cost_estimate=pl.CostEstimate(flops=2 * 10**9, bytes_accessed=10**7, transcendentals=0),
    )(hidden, recv, gain, gathered, wo, wg, wu, wd)


def body(
    tokens, memory, normalizer, stabilizer, norm_gain, w_query, w_key, w_value, w_outgate, w_input, w_forget,
    forget_bias, w_out, ffn_gain, w_gate, w_up, w_down, expert_ids, route_weights,
):
    turned = lambda w: jnp.transpose(w, (1, 2, 0))
    gain = norm_gain.reshape(1, -1)
    recv, gathered = call_a(
        tokens, gain, expert_ids.T, route_weights.T, turned(w_query), turned(w_key), turned(w_value), turned(w_outgate)
    )
    flat = recv.reshape(256, 128)
    memory_next, normalizer_next, stab_next, hidden = call_b(
        flat, tokens, gain, w_input.T, w_forget.T, forget_bias.reshape(1, 4), stabilizer, normalizer, memory
    )
    out = call_c(hidden, flat, ffn_gain.reshape(1, -1), gathered, w_out.T, w_gate[0], w_up[0], w_down[0])
    return (out, memory_next, normalizer_next, stab_next)


def solution(mesh):
    return jax.shard_map(
        body,
        mesh=mesh,
        in_specs=(
            P("ep", None),
            P("ep", "tp", None, None),
            P("ep", "tp", None),
            P("ep", "tp"),
            P(),
            P(None, "tp", "ep"),
            P(None, "tp", "ep"),
            P(None, "tp", "ep"),
            P(None, "tp", "ep"),
            P(None, "tp"),
            P(None, "tp"),
            P("tp"),
            P("tp", "ep"),
            P(),
            P("ep", None, "tp"),
            P("ep", None, "tp"),
            P("ep", "tp", None),
            P("ep", None),
            P("ep", None),
        ),
        out_specs=(P("ep", None), P("ep", "tp", None, None), P("ep", "tp", None), P("ep", "tp")),
        check_vma=False,
    )
```

```python
import functools

import jax
import jax.numpy as jnp
from jax import lax
from jax.experimental import pallas as pl
from jax.experimental.pallas import tpu as pltpu
from jax.sharding import PartitionSpec as P

MESH = pl.DeviceIdType.MESH
F32 = jnp.float32
BF16 = jnp.bfloat16
STRIDE = {"x": 1, "y": 4, "z": 16}
SEND_ORDER = (1, 3, 2)


def place():
    ep = lax.axis_index("ep")
    at = {"x": lax.rem(ep, 4), "y": lax.rem(ep // 4, 4), "z": ep // 16}
    return ep, lax.axis_index("tp"), at


def shifted(at, axis, offset):
    return lax.rem(at[axis] + 4 + offset, 4)


def peer(ep, at, axis, offset):
    return ep + (shifted(at, axis, offset) - at[axis]) * STRIDE[axis]


def remote(src, dst, send, recv, ep, tp):
    return pltpu.make_async_remote_copy(
        src_ref=src, dst_ref=dst, send_sem=send, recv_sem=recv, device_id=(ep, tp), device_id_type=MESH
    )


def greet(ep, tp, at):
    barrier = pltpu.get_barrier_semaphore()
    for axis in "xyz":
        for o in (1, 2, 3):
            pl.semaphore_signal(barrier, inc=1, device_id=(peer(ep, at, axis, o), tp), device_id_type=MESH)
    pl.semaphore_signal(barrier, inc=1, device_id=(ep, 1 - tp), device_id_type=MESH)


def met():
    pl.semaphore_wait(pltpu.get_barrier_semaphore(), 10)


ORDERS = (("x", "y", "z"), ("x", "z", "y"), ("y", "z", "x"))
PARTS = ((0, 640), (640, 640), (1280, 768))
TURN = 1280
WIDE = ((0, 1280), (1280, 1280), (2560, 1536))
WIDE_TURN = 2560


def cols_of(part):
    return pl.ds(PARTS[part][0], PARTS[part][1])


def wide_of(part):
    return pl.ds(WIDE[part][0], WIDE[part][1])


def line_of(at, part, m, n):
    first, second, third = ORDERS[part]
    c = dict(at)
    c[second] = shifted(at, second, -m)
    c[third] = shifted(at, third, -n)
    return c["z"] * 4 + (c["y"] if first == "x" else c["x"])


def first_send(ep, tp, at, part, own, slot, s1, r1):
    axis = ORDERS[part][0]
    for o in SEND_ORDER:
        remote(own, slot(at[axis]), s1.at[part, o], r1.at[part, o], peer(ep, at, axis, o), tp).start()


def first_arrived(ep, tp, at, part, own, slot, s1, r1):
    for o in SEND_ORDER:
        remote(own, slot(at[ORDERS[part][0]]), s1.at[part, o], r1.at[part, o], ep, tp).wait_recv()


def first_end(ep, tp, at, part, own, slot, s1, r1):
    for o in SEND_ORDER:
        remote(own, slot(at[ORDERS[part][0]]), s1.at[part, o], r1.at[part, o], ep, tp).wait_send()


def lines_relay(ep, tp, at, ref, part, m, n, pair):
    if pair is not None:
        here = ref(line_of(at, part, m, n), part)
        remote(here, here, pair[0].at[part, m, n], pair[1].at[part, m, n], ep, 1 - tp).start()


def lines_onward(ep, tp, at, ref, part, m, s3, r3):
    here = ref(line_of(at, part, m, 0), part)
    for o in SEND_ORDER:
        remote(here, here, s3.at[part, m, o], r3.at[part, m, o], peer(ep, at, ORDERS[part][2], o), tp).start()


def lines_early(parts, ep, tp, at, ref, s2, r2, s3, r3, pair=None):
    for part in parts:
        here = ref(line_of(at, part, 0, 0), part)
        for o in SEND_ORDER:
            remote(here, here, s2.at[part, o], r2.at[part, o], peer(ep, at, ORDERS[part][1], o), tp).start()
    for part in parts:
        lines_onward(ep, tp, at, ref, part, 0, s3, r3)
        lines_relay(ep, tp, at, ref, part, 0, 0, pair)


def lines_late(parts, ep, tp, at, ref, s2, r2, s3, r3, pair=None, seen=None):
    if seen is not None:
        for part in parts:
            seen(part, line_of(at, part, 0, 0))
    for m in SEND_ORDER:
        for part in parts:
            here = ref(line_of(at, part, m, 0), part)
            remote(here, here, s2.at[part, m], r2.at[part, m], ep, tp).wait_recv()
            lines_onward(ep, tp, at, ref, part, m, s3, r3)
            lines_relay(ep, tp, at, ref, part, m, 0, pair)
            if seen is not None:
                seen(part, line_of(at, part, m, 0))
    for m in (0, 1, 3, 2):
        for o in SEND_ORDER:
            for part in parts:
                here = ref(line_of(at, part, m, o), part)
                remote(here, here, s3.at[part, m, o], r3.at[part, m, o], ep, tp).wait_recv()
                lines_relay(ep, tp, at, ref, part, m, o, pair)
                if seen is not None:
                    seen(part, line_of(at, part, m, o))


def lines_end(parts, ep, tp, at, ref, s2, r2, s3, r3, pair=None):
    for part in parts:
        here = ref(line_of(at, part, 0, 0), part)
        for o in SEND_ORDER:
            remote(here, here, s2.at[part, o], r2.at[part, o], ep, tp).wait_send()
        for m in range(4):
            for o in SEND_ORDER:
                remote(here, here, s3.at[part, m, o], r3.at[part, m, o], ep, tp).wait_send()
            if pair is not None:
                for n in range(4):
                    remote(here, here, pair[0].at[part, m, n], pair[1].at[part, m, n], ep, 1 - tp).wait_send()


def turned_pieces():
    for z in range(4):
        for y in range(4):
            for x in range(4):
                yield 4 * z + y, 2 * x, 4 * z + x, 2 * y


def stacked(blocks, rows):
    return jnp.concatenate([block[r : r + 2] for r in rows for block in blocks], axis=0).astype(BF16)


def kernel_a(
    tok_ref, gain_ref, ids_ref, rw_ref, wq_hbm, wk_hbm, wv_hbm, wo_hbm,
    recv_ref, all_ref,
    own2, xblk, wq, wk, wv, wo, wt, acc, acc_t, squares, squares_t, comb, came, slab,
    wsem, s1, r1, s2, r2, s3, r3, ws, wr, cs, cr, sa, ra,
):
    ep, tp, at = place()
    greet(ep, tp, at)
    loads = [
        pltpu.make_async_copy(src, dst, wsem.at[n])
        for n, (src, dst) in enumerate(((wq_hbm, wq), (wk_hbm, wk), (wv_hbm, wv), (wo_hbm, wo)))
    ]
    for load in loads:
        load.start()
    mine4 = tok_ref[...].astype(F32)
    mine2 = jnp.where(tp == 0, mine4[0:2], mine4[2:4]).astype(BF16)
    own2[...] = mine2
    own = lambda part: own2.at[:, wide_of(part)]
    slot = lambda part: lambda c: xblk.at[c, :, wide_of(part)]
    met()
    for part in range(3):
        first_send(ep, tp, at, part, own(part), slot(part), s1, r1)
    for part in range(3):
        off, width = WIDE[part]
        xblk[at[ORDERS[part][0]], :, wide_of(part)] = mine2[:, off : off + width]
    ref = lambda line, part: all_ref.at[line, :, wide_of(part)]
    lines = (ep, tp, at, ref, s2, r2, s3, r3)

    def stack(part):
        line = line_of(at, part, 0, 0)
        off, width = WIDE[part]
        for n in range(off, off + width, 256):
            cols = pl.ds(n, 256)
            all_ref[line, :, cols] = stacked([xblk[c, :, cols].astype(F32) for c in range(4)], (0,))

    for part in range(3):
        first_arrived(ep, tp, at, part, own(part), slot(part), s1, r1)
        stack(part)
        lines_early((part,), *lines)
    for load in loads:
        load.wait()
    for side in range(2):
        wt[side, 96:128, :] = jnp.zeros((32, 4096), BF16)
    for n in range(0, 4096, 1024):
        cols = pl.ds(n, 1024)
        for row, tall, w in ((0, 16, wq), (16, 16, wk), (32, 32, wv), (64, 32, wo)):
            wt[tp, row : row + tall, cols] = jnp.concatenate([w[h, :, cols].astype(F32) for h in range(4)], axis=0).astype(BF16)
    share = remote(wt.at[tp, pl.ds(0, 96), :], wt.at[tp, pl.ds(0, 96), :], ws, wr, ep, 1 - tp)
    share.start()
    squares[...] = jnp.zeros((16, 8, 128), F32)
    squares_t[...] = jnp.zeros((16, 8, 128), F32)

    def measured(part, line):
        into = squares_t if part == 2 else squares
        off, width = WIDE[part]
        total = into[line]
        for n in range(off, off + width, 128):
            v = all_ref[line, :, pl.ds(n, 128)].astype(F32)
            total += v * v
        into[line] = total

    lines_late((0, 1, 2), *lines, seen=measured)
    for line, row, line_t, row_t in turned_pieces():
        both = squares[line, row : row + 2] + squares_t[line_t, row_t : row_t + 2]
        squares[line, row : row + 2] = both
        squares_t[line_t, row_t : row_t + 2] = both

    def scale_from(sums):
        mean = jnp.sum(sums[...].reshape(128, 128), axis=-1, keepdims=True) * (1.0 / 4096)
        return lax.rsqrt(mean + 1e-06)

    scale, scale_t = scale_from(squares), scale_from(squares_t)
    share.wait_send()
    remote(wt.at[1 - tp, pl.ds(0, 96), :], wt.at[1 - tp, pl.ds(0, 96), :], ws, wr, ep, 1 - tp).wait_recv()

    def project(off, width, rows_scale):
        cols = pl.ds(off, width)
        x = all_ref[:, :, cols].astype(F32).reshape(128, width)
        normed = (x * rows_scale * gain_ref[:, cols]).astype(BF16)
        right = wt[:, :, cols].reshape(256, width)
        return lax.dot_general(normed, right, (((1,), (1,)), ((), ())), preferred_element_type=F32)

    acc[...] = project(0, WIDE_TURN, scale)
    acc_t[...] = project(WIDE_TURN, 1536, scale_t)
    for e, (line, row, line_t, row_t) in enumerate(turned_pieces()):
        a0, b0 = 8 * line + row, 8 * line_t + row_t
        for side in range(2):
            cols = slice(128 * side, 128 * side + 128)
            comb[side, e] = acc[a0 : a0 + 2, cols] + acc_t[b0 : b0 + 2, cols]
    trade = remote(comb.at[1 - tp], came, cs, cr, ep, 1 - tp)
    trade.start()
    lane = lax.broadcasted_iota(jnp.int32, (4, 128), 1)
    diagonal = lax.broadcasted_iota(jnp.int32, (4, 4), 0) == lax.broadcasted_iota(jnp.int32, (4, 4), 1)
    upright = lambda row: jnp.sum(jnp.where(diagonal, row, 0.0), axis=1, keepdims=True)
    ids = ids_ref[...].astype(F32)
    id0, id1 = upright(ids[0:1]), upright(ids[1:2])
    rw0, rw1 = upright(rw_ref[0:1, :]), upright(rw_ref[1:2, :])
    trade.wait()
    for e in range(64):
        here, there = comb[tp, e], came[e]
        columns = jnp.concatenate([jnp.where(tp == 0, here, there), jnp.where(tp == 0, there, here)], axis=0)
        weight = jnp.where(id0 == float(e), rw0, 0.0) + jnp.where(id1 == float(e), rw1, 0.0)
        slab[e] = jnp.where(lane < 96, columns, jnp.where(lane == 96, weight, 0.0))

    @pl.loop(1, 64)
    def _(o):
        to = ep ^ o
        remote(slab.at[to], recv_ref.at[ep], sa.at[o], ra.at[o], to, tp).start()

    recv_ref[ep] = slab[ep]
    for part in range(3):
        first_end(ep, tp, at, part, own(part), slot(part), s1, r1)
    lines_end((0, 1, 2), *lines)
    for z in range(4):
        for n in range(WIDE_TURN, 4096, 256):
            cols = pl.ds(n, 256)
            four = [all_ref[4 * z + x, :, cols].astype(F32) for x in range(4)]
            for y in range(4):
                all_ref[4 * z + y, :, cols] = stacked(four, (2 * y,))

    @pl.loop(1, 64)
    def _(o):
        remote(slab.at[ep ^ o], recv_ref.at[ep ^ o], sa.at[o], ra.at[o], ep ^ o, tp).wait()


def log_sigmoid(v):
    return -(jnp.maximum(-v, 0.0) + jnp.log1p(jnp.exp(-jnp.abs(v))))


def one_hot(rows, cols, test):
    r = lax.broadcasted_iota(jnp.int32, (rows, cols), 0)
    c = lax.broadcasted_iota(jnp.int32, (rows, cols), 1)
    return test(r, c)


def kernel_b(
    recv_ref, tok_ref, gain_ref, win_ref, wfg_ref, fbias_ref, stab_ref, nrm_ref, mem_hbm,
    memn_hbm, nrmn_ref, stabn_ref, hid_ref,
    buf, kq, hids, isem, osem,
):
    ins = [pltpu.make_async_copy(mem_hbm.at[n // 4, n % 4], buf.at[n], isem.at[n]) for n in range(16)]
    outs = [pltpu.make_async_copy(buf.at[n], memn_hbm.at[n // 4, n % 4], osem.at[n]) for n in range(16)]
    for copy in ins:
        copy.start()
    x = tok_ref[...].astype(F32)
    scale = lax.rsqrt(jnp.mean(x * x, axis=-1, keepdims=True) + 1e-06)
    normed = (x * scale * gain_ref[...]).astype(BF16).astype(F32)
    lane = lax.broadcasted_iota(jnp.int32, (4, 4), 1)
    in_pre = jnp.zeros((4, 4), F32)
    forget = jnp.zeros((4, 4), F32)
    for h in range(4):
        i_h = jnp.sum(normed * win_ref[h : h + 1, :].astype(F32), axis=-1, keepdims=True)
        f_h = jnp.sum(normed * wfg_ref[h : h + 1, :].astype(F32), axis=-1, keepdims=True)
        in_pre = jnp.where(lane == h, i_h, in_pre)
        forget = jnp.where(lane == h, f_h, forget)
    log_forget = log_sigmoid(forget + fbias_ref[...])
    held = log_forget + stab_ref[...]
    stab_next = jnp.maximum(held, in_pre)
    decay = jnp.exp(held - stab_next)
    inweight = jnp.exp(in_pre - stab_next)
    floor = jnp.exp(-stab_next)
    stabn_ref[...] = stab_next

    e4 = one_hot(256, 64, lambda r, c: r // 4 == c).astype(BF16)
    e8 = one_hot(512, 64, lambda r, c: r // 8 == c).astype(BF16)
    keep4 = one_hot(256, 128, lambda r, c: (r % 4 == c % 4) & (c < 32))
    keep8 = one_hot(512, 128, lambda r, c: (r % 8 == c % 8) & (c >= 32) & (c < 96))
    vo_cols = jnp.zeros((512, 128), F32)
    qk_cols = jnp.zeros((256, 128), F32)
    wide = []
    for h in range(4):
        wide.append(one_hot(128, 256, lambda r, c: (r // 4 == jnp.where(c < 128, 4 + h, h)) & (r < 32)).astype(BF16))
    for t in range(4):
        rows = recv_ref[pl.ds(t, 64, stride=4), :].astype(BF16)
        y4 = jnp.where(keep4, jnp.dot(e4, rows, preferred_element_type=F32), 0.0).astype(BF16)
        y8 = jnp.where(keep8, jnp.dot(e8, rows, preferred_element_type=F32), 0.0).astype(BF16)
        for h in range(4):
            kq[t * 4 + h] = jnp.dot(y4, wide[h], preferred_element_type=F32)
        f4 = one_hot(128, 128, lambda r, c: (c == t * 8 + r // 4) & (r < 32)).astype(BF16)
        f8 = one_hot(128, 128, lambda r, c: (c == t * 8 + (r - 32) // 8) & (r >= 32) & (r < 96)).astype(BF16)
        qk_cols += jnp.dot(y4, f4, preferred_element_type=F32)
        vo_cols += jnp.dot(y8, f8, preferred_element_type=F32)
    qk_rows = qk_cols.T
    vo_rows = vo_cols.T
    for n in range(16):
        t, h = n // 4, n % 4
        d = decay[t : t + 1, h : h + 1]
        w = inweight[t : t + 1, h : h + 1]
        q_row = qk_rows[t * 8 + h : t * 8 + h + 1, :] * 0.0625
        k_row = qk_rows[t * 8 + 4 + h : t * 8 + 5 + h, :]
        v_row = vo_rows[t * 8 + h : t * 8 + h + 1, :]
        o_row = vo_rows[t * 8 + 4 + h : t * 8 + 5 + h, :]
        norm_next = d * nrm_ref[t, h : h + 1, :] + w * k_row
        nrmn_ref[t, h : h + 1, :] = norm_next
        den = jnp.sum(q_row * norm_next, axis=-1, keepdims=True)
        ins[n].wait()
        d_all = jnp.broadcast_to(d, (8, 128))
        vs = [jnp.broadcast_to(w * v_row[:, 128 * c : 128 * c + 128], (8, 128)) for c in range(4)]

        def step(r, total, n=n, d_all=d_all, vs=vs):
            total = list(total)
            for g in range(4):
                rows = pl.ds(pl.multiple_of(r * 32 + 8 * g, 8), 8)
                k_all = kq[n, rows, 0:128]
                q_all = kq[n, rows, 128:256]
                for c in range(4):
                    cols = slice(128 * c, 128 * c + 128)
                    new = d_all * buf[n, rows, cols] + k_all * vs[c]
                    buf[n, rows, cols] = new
                    total[c] = total[c] + q_all * new
            return tuple(total)

        total = lax.fori_loop(0, 8, step, tuple(jnp.zeros((8, 128), F32) for _ in range(4)), unroll=True)
        outs[n].start()
        numer = jnp.sum(jnp.concatenate(total, axis=1), axis=0, keepdims=True) * 0.0625
        hidden = numer / jnp.maximum(jnp.abs(den), floor[t : t + 1, h : h + 1]) * jax.nn.sigmoid(o_row)
        hids[t : t + 1, h * 512 : (h + 1) * 512] = hidden
    hid_ref[...] = hids[...].astype(BF16)
    for copy in outs:
        copy.wait()


def kernel_c(
    hid_ref, recv_ref, gain_ref, tok_hbm, wo_hbm, wg_hbm, wu_hbm, wd_hbm,
    out_ref,
    xblk, hall, wo, toks, wg, wu, wd, pre, pre_t, pk, pr_in, mall, resid, squares, gate, up, act, act_t,
    weights, weights_t, terms, r1buf, s1buf, r2buf, xsend, xrecv, ends,
    wsem, s1, r1, s2, r2, s3, r3, ms1, mr1, ms2, mr2, ms3, mr3, es, er, hs, hr,
    q1s, q1r, q2s, q2r, q3s, q3r, fs, fr,
):
    ep, tp, at = place()
    greet(ep, tp, at)
    shared = ((wg_hbm, wg), (wu_hbm, wu), (wd_hbm, wd))
    loads = [pltpu.make_async_copy(wo_hbm, wo, wsem.at[0]), pltpu.make_async_copy(tok_hbm, toks, wsem.at[1])]
    loads += [pltpu.make_async_copy(src, dst.at[tp], wsem.at[2 + n]) for n, (src, dst) in enumerate(shared)]
    for load in loads:
        load.start()
    own = lambda part: hid_ref.at[:, cols_of(part)]
    slot = lambda part: lambda c: xblk.at[c, :, cols_of(part)]
    met()
    for part in range(3):
        first_send(ep, tp, at, part, own(part), slot(part), s1, r1)
    gifts = [remote(src, dst.at[tp], es.at[n], er.at[n], ep, 1 - tp) for n, (src, dst) in enumerate(shared)]
    for gift in gifts:
        gift.start()
    for part in range(3):
        xblk[at[ORDERS[part][0]], :, cols_of(part)] = hid_ref[:, cols_of(part)]
    href = lambda line, part: hall.at[line, :, cols_of(part)]
    hidden_lines = (ep, tp, at, href, s2, r2, s3, r3)
    for part in range(3):
        first_arrived(ep, tp, at, part, own(part), slot(part), s1, r1)
        off, width = PARTS[part]
        for n in range(off, off + width, 128):
            cols = pl.ds(n, 128)
            hall[line_of(at, part, 0, 0), :, cols] = stacked([xblk[c, :, cols].astype(F32) for c in range(4)], (0, 2))
        lines_early((part,), *hidden_lines)
    for load in loads:
        load.wait()
    squares[...] = jnp.zeros((128, 128), F32)
    for t in range(2):
        weights[pl.ds(t, 64, stride=2), :] = jnp.where(
            tp == 0, recv_ref[pl.ds(t, 64, stride=4), :], recv_ref[pl.ds(2 + t, 64, stride=4), :]
        )
    for line, row, line_t, row_t in turned_pieces():
        a0, b0 = 8 * line + row, 8 * line_t + row_t
        weights_t[b0 : b0 + 2, :] = weights[a0 : a0 + 2, :]
    r = lax.broadcasted_iota(jnp.int32, (128, 128), 0)
    c = lax.broadcasted_iota(jnp.int32, (128, 128), 1)
    turn = (c == (r // 32) * 32 + (r // 2 % 4) * 8 + (r // 8 % 4) * 2 + r % 2).astype(BF16)
    lines_late((0, 1, 2), *hidden_lines)

    def onto(off, width):
        left = hall[:, :, pl.ds(off, width)].reshape(256, width)
        return lax.dot_general(left, wo[:, pl.ds(off, width)], (((1,), (1,)), ((), ())), preferred_element_type=F32)

    pre[...] = onto(0, TURN).reshape(16, 16, 64)
    pre_t[...] = onto(TURN, 768).reshape(16, 16, 64)
    for core in range(2):
        for line, row, line_t, row_t in turned_pieces():
            a0, b0 = 8 * core + row, 8 * core + row_t
            pre[line, a0 : a0 + 2] += pre_t[line_t, b0 : b0 + 2]
        sides = [pre[8 * k : 8 * k + 8, 8 * core : 8 * core + 8].reshape(64, 64) for k in range(2)]
        pk[core] = jnp.concatenate(sides, axis=1).astype(BF16)
    swap = remote(pk.at[1 - tp], pr_in, hs, hr, ep, 1 - tp)
    swap.start()
    for part in range(3):
        first_end(ep, tp, at, part, own(part), slot(part), s1, r1)
    lines_end((0, 1, 2), *hidden_lines)
    swap.wait()
    mine = at["z"] * 4 + at["y"]
    mall[mine, at["x"]] = (pk[tp].astype(F32) + pr_in[...].astype(F32)).astype(BF16)
    both = (0, 1)
    mown = lambda part: mall.at[mine, at["x"], pl.ds(32 * part, 32), :]
    mslot = lambda part: lambda c: mall.at[mine, c, pl.ds(32 * part, 32), :]
    for part in both:
        first_send(ep, tp, at, part, mown(part), mslot(part), ms1, mr1)
    mref = lambda line, part: mall.at[line, :, pl.ds(32 * part, 32), :]
    mixed_lines = (ep, tp, at, mref, ms2, mr2, ms3, mr3)
    for part in both:
        first_arrived(ep, tp, at, part, mown(part), mslot(part), ms1, mr1)
        lines_early((part,), *mixed_lines)

    low = lax.broadcasted_iota(jnp.int32, (32, 128), 1) < 64

    def joined(part, line):
        rows = [slice(64 * k + 32 * part, 64 * k + 32 * part + 32) for k in range(2)]
        total = [squares[rows[k], :] for k in range(2)]
        for i in range(2):
            a = mall[line, 2 * i, 32 * part : 32 * part + 32, :].astype(F32)
            b = mall[line, 2 * i + 1, 32 * part : 32 * part + 32, :].astype(F32)
            mixes = (jnp.where(low, a, pltpu.roll(b, 64, 1)), jnp.where(low, pltpu.roll(a, 64, 1), b))
            cols = pl.ds(pl.multiple_of(256 * line + 128 * i, 128), 128)
            for k in range(2):
                first = 8 * k + 4 * part
                summed = toks[first : first + 4, :, cols].astype(F32).reshape(32, 128) + mixes[k]
                resid[rows[k], cols] = summed
                total[k] += summed * summed
        for k in range(2):
            squares[rows[k], :] = total[k]

    lines_late(both, *mixed_lines, seen=joined)
    scale = lax.rsqrt(jnp.sum(squares[...], axis=-1, keepdims=True) * (1.0 / 4096) + 1e-06)
    for n in range(3):
        gifts[n].wait_send()
        remote(wg_hbm, shared[n][1].at[1 - tp], es.at[n], er.at[n], ep, 1 - tp).wait_recv()
    for n in range(0, 4096, 1024):
        cols = pl.ds(n, 1024)
        x = (resid[:, cols] * scale * gain_ref[:, cols]).astype(BF16)
        for k in range(2):
            g = jnp.dot(x, wg[k, cols, :], preferred_element_type=F32)
            u = jnp.dot(x, wu[k, cols, :], preferred_element_type=F32)
            if n == 0:
                gate[k] = g
                up[k] = u
            else:
                gate[k] += g
                up[k] += u
    for k in range(2):
        g = gate[k]
        act[k] = (g * jax.nn.sigmoid(g) * up[k]).astype(BF16)
        act_t[k] = jnp.dot(turn, act[k], preferred_element_type=F32).astype(BF16)

    r1_at = lambda part, o: r1buf.at[part, o, :, :, pl.ds(0, WIDE[part][1])]
    for part in (2, 0, 1):
        off, width = WIDE[part]
        left, by = (act_t, weights_t) if part == 2 else (act, weights)
        for n in range(off, off + width, 256):
            cols = pl.ds(n, 256)
            t0 = jnp.dot(left[0], wd[0, :, cols], preferred_element_type=F32).astype(BF16).astype(F32)
            t1 = jnp.dot(left[1], wd[1, :, cols], preferred_element_type=F32).astype(BF16).astype(F32)
            terms[:, :, :, cols] = ((t0 + t1) * by[:, 96:97]).reshape(4, 4, 8, 256).astype(BF16)
        axis = ORDERS[part][2]
        for o in SEND_ORDER:
            k = shifted(at, axis, o)
            src = terms.at[k, :, :, wide_of(part)] if part == 0 else terms.at[:, k, :, wide_of(part)]
            remote(src, r1_at(part, o), q1s.at[part, o], q1r.at[part, o], peer(ep, at, axis, o), tp).start()
    for part in both:
        first_end(ep, tp, at, part, mown(part), mslot(part), ms1, mr1)
    lines_end(both, *mixed_lines)

    s1_at = lambda part, k: s1buf.at[part, k, :, pl.ds(0, WIDE[part][1])]
    r2_at = lambda part, o: r2buf.at[part, o, :, pl.ds(0, WIDE[part][1])]
    for part in (2, 0, 1):
        off, width = WIDE[part]
        for o in SEND_ORDER:
            remote(r1_at(part, 0), r1_at(part, o), q1s.at[part, o], q1r.at[part, o], ep, tp).wait_recv()
        for n in range(0, width, 256):
            cols = pl.ds(off + n, 256)
            mine_term = terms[at["z"], :, :, cols] if part == 0 else terms[:, at[ORDERS[part][2]], :, cols]
            total = mine_term.astype(F32)
            for o in (1, 2, 3):
                total += r1buf[part, o, :, :, pl.ds(n, 256)].astype(F32)
            s1buf[part, :, :, pl.ds(n, 256)] = total.astype(BF16)
        axis = ORDERS[part][1]
        for o in SEND_ORDER:
            remote(s1_at(part, shifted(at, axis, o)), r2_at(part, o), q2s.at[part, o], q2r.at[part, o], peer(ep, at, axis, o), tp).start()
    for part in (2, 0, 1):
        off, width = WIDE[part]
        for o in SEND_ORDER:
            remote(s1_at(part, 0), r2_at(part, o), q2s.at[part, o], q2r.at[part, o], ep, tp).wait_recv()
        for n in range(0, width, 256):
            total = s1buf[part, at[ORDERS[part][1]], :, pl.ds(n, 256)].astype(F32)
            for o in (1, 2, 3):
                total += r2buf[part, o, :, pl.ds(n, 256)].astype(F32)
            for k in range(4):
                xsend[k, :, pl.ds(off + n, 256)] = total[2 * k : 2 * k + 2].astype(BF16)
        axis = ORDERS[part][0]
        for o in SEND_ORDER:
            there = xsend.at[shifted(at, axis, o), :, wide_of(part)]
            remote(there, xrecv.at[o, :, wide_of(part)], q3s.at[part, o], q3r.at[part, o], peer(ep, at, axis, o), tp).start()
    for part in (2, 0, 1):
        off, width = WIDE[part]
        cols = wide_of(part)
        eight = resid[pl.ds(pl.multiple_of(8 * mine, 8), 8), cols]
        total = eight[0:2]
        for k in range(1, 4):
            total = jnp.where(at["x"] == k, eight[2 * k : 2 * k + 2], total)
        total = total + xsend[at[ORDERS[part][0]], :, cols].astype(F32)
        for o in SEND_ORDER:
            remote(xsend.at[0, :, cols], xrecv.at[o, :, cols], q3s.at[part, o], q3r.at[part, o], ep, tp).wait_recv()
            total += xrecv[o, :, cols].astype(F32)
        ends[tp, :, cols] = total.astype(BF16)
    last = remote(ends.at[tp], ends.at[tp], fs, fr, ep, 1 - tp)
    last.start()
    for part in range(3):
        for o in SEND_ORDER:
            remote(r1_at(part, 0), r1_at(part, o), q1s.at[part, o], q1r.at[part, o], ep, tp).wait_send()
            remote(s1_at(part, 0), r2_at(part, o), q2s.at[part, o], q2r.at[part, o], ep, tp).wait_send()
            there = xsend.at[0, :, wide_of(part)]
            remote(there, xrecv.at[o, :, wide_of(part)], q3s.at[part, o], q3r.at[part, o], ep, tp).wait_send()
    last.wait_send()
    remote(ends.at[1 - tp], ends.at[1 - tp], fs, fr, ep, 1 - tp).wait_recv()
    for n in range(0, 4096, 1024):
        cols = pl.ds(n, 1024)
        out_ref[:, cols] = jnp.concatenate([ends[k, :, cols].astype(F32) for k in range(2)], axis=0).astype(BF16)


V = pl.BlockSpec(memory_space=pltpu.VMEM)
ANY = pl.BlockSpec(memory_space=pl.ANY)
DMA = pltpu.SemaphoreType.DMA


def shape(dims, dtype):
    return jax.ShapeDtypeStruct(dims, dtype)


def call_a(tokens, gain, ids, rw, wq, wk, wv, wo):
    return pl.pallas_call(
        kernel_a,
        name="gather_project",
        out_shape=(shape((64, 4, 128), F32), shape((16, 8, 4096), BF16)),
        in_specs=[V, V, V, V, ANY, ANY, ANY, ANY],
        out_specs=(V, V),
        scratch_shapes=[
            pltpu.VMEM((2, 4096), BF16),
            pltpu.VMEM((4, 2, 4096), BF16),
            pltpu.VMEM((4, 4, 4096), BF16),
            pltpu.VMEM((4, 4, 4096), BF16),
            pltpu.VMEM((4, 8, 4096), BF16),
            pltpu.VMEM((4, 8, 4096), BF16),
            pltpu.VMEM((2, 128, 4096), BF16),
            pltpu.VMEM((128, 256), F32),
            pltpu.VMEM((128, 256), F32),
            pltpu.VMEM((16, 8, 128), F32),
            pltpu.VMEM((16, 8, 128), F32),
            pltpu.VMEM((2, 64, 2, 128), F32),
            pltpu.VMEM((64, 2, 128), F32),
            pltpu.VMEM((64, 4, 128), F32),
            DMA((4,)),
            DMA((3, 4)), DMA((3, 4)),
            DMA((3, 4)), DMA((3, 4)),
            DMA((3, 4, 4)), DMA((3, 4, 4)),
            DMA(()), DMA(()), DMA(()), DMA(()),
            DMA((64,)), DMA((64,)),
        ],
        compiler_params=pltpu.CompilerParams(collective_id=0, has_side_effects=True),
        cost_estimate=pl.CostEstimate(flops=10**9, bytes_accessed=10**7, transcendentals=0),
    )(tokens, gain, ids, rw, wq, wk, wv, wo)


def call_b(recv, tokens, gain, win, wfg, fbias, stab, nrm, mem):
    return pl.pallas_call(
        kernel_b,
        name="cell",
        out_shape=(
            shape(mem.shape, F32), shape(nrm.shape, F32), shape(stab.shape, F32), shape((4, 2048), BF16),
        ),
        in_specs=[V, V, V, V, V, V, V, V, ANY],
        out_specs=(ANY, V, V, V),
        scratch_shapes=[
            pltpu.VMEM((16, 256, 512), F32),
            pltpu.VMEM((16, 256, 256), F32),
            pltpu.VMEM((4, 2048), F32),
            DMA((16,)), DMA((16,)),
        ],
        compiler_params=pltpu.CompilerParams(),
        cost_estimate=pl.CostEstimate(flops=10**8, bytes_accessed=2 * 10**7, transcendentals=0),
    )(recv, tokens, gain, win, wfg, fbias, stab, nrm, mem)


def call_c(hidden, recv, gain, gathered, wo, wg, wu, wd):
    lines = lambda k: [DMA((k, 4)), DMA((k, 4)), DMA((k, 4)), DMA((k, 4)), DMA((k, 4, 4)), DMA((k, 4, 4))]
    return pl.pallas_call(
        kernel_c,
        name="experts",
        out_shape=shape((4, 4096), BF16),
        in_specs=[V, V, V, ANY, ANY, ANY, ANY, ANY],
        out_specs=V,
        scratch_shapes=[
            pltpu.VMEM((4, 4, 2048), BF16),
            pltpu.VMEM((16, 16, 2048), BF16),
            pltpu.VMEM((64, 2048), BF16),
            pltpu.VMEM((16, 8, 4096), BF16),
            pltpu.VMEM((2, 4096, 256), BF16),
            pltpu.VMEM((2, 4096, 256), BF16),
            pltpu.VMEM((2, 256, 4096), BF16),
            pltpu.VMEM((16, 16, 64), F32),
            pltpu.VMEM((16, 16, 64), F32),
            pltpu.VMEM((2, 64, 128), BF16),
            pltpu.VMEM((64, 128), BF16),
            pltpu.VMEM((16, 4, 64, 128), BF16),
            pltpu.VMEM((128, 4096), F32),
            pltpu.VMEM((128, 128), F32),
            pltpu.VMEM((2, 128, 256), F32),
            pltpu.VMEM((2, 128, 256), F32),
            pltpu.VMEM((2, 128, 256), BF16),
            pltpu.VMEM((2, 128, 256), BF16),
            pltpu.VMEM((128, 128), F32),
            pltpu.VMEM((128, 128), F32),
            pltpu.VMEM((4, 4, 8, 4096), BF16),
            pltpu.VMEM((3, 4, 4, 8, 1536), BF16),
            pltpu.VMEM((3, 4, 8, 1536), BF16),
            pltpu.VMEM((3, 4, 8, 1536), BF16),
            pltpu.VMEM((4, 2, 4096), BF16),
            pltpu.VMEM((4, 2, 4096), BF16),
            pltpu.VMEM((2, 2, 4096), BF16),
            DMA((5,)),
            *lines(3),
            *lines(2), DMA((3,)), DMA((3,)),
            DMA(()), DMA(()),
            DMA((3, 4)), DMA((3, 4)), DMA((3, 4)), DMA((3, 4)), DMA((3, 4)), DMA((3, 4)), DMA(()), DMA(()),
        ],
        compiler_params=pltpu.CompilerParams(collective_id=1, has_side_effects=True),
        cost_estimate=pl.CostEstimate(flops=2 * 10**9, bytes_accessed=10**7, transcendentals=0),
    )(hidden, recv, gain, gathered, wo, wg, wu, wd)


def body(
    tokens, memory, normalizer, stabilizer, norm_gain, w_query, w_key, w_value, w_outgate, w_input, w_forget,
    forget_bias, w_out, ffn_gain, w_gate, w_up, w_down, expert_ids, route_weights,
):
    turned = lambda w: jnp.transpose(w, (1, 2, 0))
    gain = norm_gain.reshape(1, -1)
    recv, gathered = call_a(
        tokens, gain, expert_ids.T, route_weights.T, turned(w_query), turned(w_key), turned(w_value), turned(w_outgate)
    )
    flat = recv.reshape(256, 128)
    memory_next, normalizer_next, stab_next, hidden = call_b(
        flat, tokens, gain, w_input.T, w_forget.T, forget_bias.reshape(1, 4), stabilizer, normalizer, memory
    )
    out = call_c(hidden, flat, ffn_gain.reshape(1, -1), gathered, w_out.T, w_gate[0], w_up[0], w_down[0])
    return (out, memory_next, normalizer_next, stab_next)


def solution(mesh):
    return jax.shard_map(
        body,
        mesh=mesh,
        in_specs=(
            P("ep", None),
            P("ep", "tp", None, None),
            P("ep", "tp", None),
            P("ep", "tp"),
            P(),
            P(None, "tp", "ep"),
            P(None, "tp", "ep"),
            P(None, "tp", "ep"),
            P(None, "tp", "ep"),
            P(None, "tp"),
            P(None, "tp"),
            P("tp"),
            P("tp", "ep"),
            P(),
            P("ep", None, "tp"),
            P("ep", None, "tp"),
            P("ep", "tp", None),
            P("ep", None),
            P("ep", None),
        ),
        out_specs=(P("ep", None), P("ep", "tp", None, None), P("ep", "tp", None), P("ep", "tp")),
        check_vma=False,
    )
```
